32 devices in a mesh: ep: 16 (over z, y, x), tp: 2 (over core).
Axes of the slice: x: 2, y: 2, z: 4, core: 2. Of those that a mesh axis runs over, the one named last changes fastest.
Arguments:
- hidden: bfloat16 [1024, 2048], P('ep'), may hold values from -6 to 6
- mix_gain: float32 [2048], replicated, may hold values from 0.1 to 1.9
- recept_weight: bfloat16 [2048, 1024], P(None, 'tp'), may hold values from -0.125 to 0.125
- key_weight: bfloat16 [2048, 1024], P(None, 'tp'), may hold values from -0.125 to 0.125
- value_weight: bfloat16 [2048, 1024], P(None, 'tp'), may hold values from -0.125 to 0.125
- decay_down: bfloat16 [2048, 64], replicated, may hold values from -0.125 to 0.125
- decay_up: bfloat16 [64, 1024], replicated, may hold values from -0.75 to 0.75
- decay_bias: float32 [1024], replicated, may hold values from -4 to 1
- rate_down: bfloat16 [2048, 64], replicated, may hold values from -0.125 to 0.125
- rate_up: bfloat16 [64, 1024], replicated, may hold values from -0.75 to 0.75
- rate_bias: float32 [1024], replicated, may hold values from -4 to 4
- head_gain: float32 [1024], replicated, may hold values from 0.1 to 1.9
- out_weight: bfloat16 [1024, 2048], P('tp'), may hold values from -0.1875 to 0.1875
- memory_state: float32 [1024, 16, 64, 64], P('ep', 'tp'), may hold values from -6 to 6
- ffn_gain: float32 [2048], replicated, may hold values from 0.1 to 1.9
- blend_vector: bfloat16 [2048], replicated, may hold values from -0.125 to 0.125
- dense_gate: bfloat16 [2048, 5632], P(None, ('ep', 'tp')), may hold values from -0.125 to 0.125
- dense_up: bfloat16 [2048, 5632], P(None, ('ep', 'tp')), may hold values from -0.125 to 0.125
- dense_down: bfloat16 [5632, 2048], P(('ep', 'tp')), may hold values from -0.3125 to 0.3125
- expert_gate: bfloat16 [16, 2048, 1536], P('ep', None, 'tp'), may hold values from -0.125 to 0.125
- expert_up: bfloat16 [16, 2048, 1536], P('ep', None, 'tp'), may hold values from -0.125 to 0.125
- expert_down: bfloat16 [16, 1536, 2048], P('ep', 'tp'), may hold values from -0.15625 to 0.15625
- routing: int32 [1024, 2], P('ep'), may hold values from 0 to 15, all different within a row; in each aligned block of 64 rows (0 to 63, 64 to 127, ...) at most 16 rows name the same one
- route_scale: float32 [1024, 2], P('ep'), may hold values from 0.25 to 1
Outputs:
- layer_out: bfloat16 [1024, 2048], P('ep')
- new_state: float32 [1024, 16, 64, 64], P('ep', 'tp')
The draws below stay inside these ranges and needn't reach their ends.
Inputs may be any that keep to these rules, and one draw needn't show every extreme that they name: `routing`: among the 64 sequences of one index of ep, no expert is chosen more than 16 times, and some expert is chosen exactly 16 times; a sequence's 2 choices differ.
All inputs are finite; a program needn't handle non-finite values.
Results may differ from the reference program's by a relative error of at most 0.017.
Values may be sent and summed in bfloat16 or wider, within the bound.
No kernel may reach another device: no remote copies, remote signals or barrier semaphores. Data moves between devices by JAX's collectives and lax.ppermute only.
A program may use at most 192 MiB of HBM per device.

```python
import math
import jax
import jax.numpy as jnp
import numpy as np
from jax import lax

D = 2048
HEADS = 16
HEAD = 64
LOW = 64
DFF = 5632
EFF = 1536
TOPK = 2
SEQS = 64
SEQUENCES = 1024
EXPERTS = 16
CAP = 16
N_EP = 16
N_TP = 2


def block_scale(stream_key, dims, pieces, least, largest):
    def one(position, blocks):
        steps = jax.random.uniform(jax.random.fold_in(jax.random.fold_in(stream_key, 6), position), (blocks,), jnp.float32, least / len(pieces), largest / len(pieces))
        return jnp.repeat(jnp.exp(steps), dims[position] // blocks).reshape((-1,) + (1,) * (len(dims) - position - 1))

    factor_of = one(*pieces[0])
    for cut in pieces[1:]:
        factor_of = factor_of * one(*cut)
    return factor_of


def assign_block(own_key, own, number, rows, number_of, top, most, lean):
    ranking = jax.random.permutation(own_key, number_of)
    packed, common = portions_of(number_of, rows * top, most, lean, True), portions_of(number_of, rows * top, most, lean, False)
    places = jnp.arange(number_of)

    def named(sizes, offset_by):
        used = int((sizes > 0).sum())
        fixed = max(1, used // 4)
        passed = fixed + (places - fixed + offset_by * (used - fixed)) % max(1, number_of - fixed)
        return jnp.zeros((number_of,), jnp.int32).at[ranking[jnp.where(places < fixed, places, passed)]].set(jnp.asarray(sizes, jnp.int32))

    sizes = jnp.where(number % 4 == 0, named(packed, number // 4), named(common, number - number // 4 - 1))
    mixed = jax.random.permutation(jax.random.fold_in(own, 3), number_of)
    donor, receiver = mixed[0:number_of // 2 * 2:2], mixed[1:number_of // 2 * 2:2]
    slack = jnp.minimum(sizes[donor] - 1, most - sizes[receiver]) // 2
    slack = jnp.where((donor == ranking[0]) | (receiver == ranking[0]) | (sizes[receiver] == 0), 0, jnp.maximum(slack, 0))
    passed = jax.random.randint(jax.random.fold_in(own, 4), (number_of // 2,), 0, 1 << 20) % (slack + 1)
    sizes = sizes.at[donor].add(-passed).at[receiver].add(passed)
    members = jnp.searchsorted(jnp.cumsum(sizes), jnp.arange(rows * top), side="right").astype(jnp.int32)
    listing = members.reshape(top, rows).T
    listing = listing[jax.random.permutation(jax.random.fold_in(own, 1), rows)]
    offset_by = jax.random.randint(jax.random.fold_in(own, 2), (rows, 1), 0, top)
    return jnp.take_along_axis(listing, (jnp.arange(top)[None, :] + offset_by) % top, axis=1)


def portions_of(count, total, most, lean, full):
    portions = [(1 << 20) // math.isqrt(grade ** lean) + 1 for grade in range(1, count + 1)]
    largest = most if full else min(most, max(-(-total // count), total * portions[0] // sum(portions)))
    least = 1 if total - largest >= count - 1 else 0
    counts, rest = [largest] + [least] * (count - 1), total - largest - least * (count - 1)
    while rest > 0:
        movable = [i for i in range(1, count) if counts[i] < largest] or [i for i in range(1, count) if counts[i] < most]
        pool, remaining = sum([portions[i] for i in movable]), rest
        for i in movable:
            extra = min(most - counts[i], max(1, remaining * portions[i] // pool), rest)
            counts[i] = counts[i] + extra
            rest = rest - extra
    return np.array(counts)


def scatter_about(key, shape, width, bound, pieces=(), held_as=jnp.bfloat16):
    values = jax.random.normal(key, shape, jnp.float32) * width
    if len(pieces) > 0:
        values = block_scale(key, shape, pieces, -0.22, 0.18) * values
    return jnp.clip(values, min=-bound, max=bound).astype(held_as)


def setup_inputs(seed: int = 0) -> dict:
    arg_keys = jax.random.split(jax.random.key(seed), 25)
    hidden = scatter_about(arg_keys[0], (SEQUENCES, D), 1.0, 6.0, ((0, 16),))
    mix_gain = jnp.clip(1.0 + 0.18 * jax.random.normal(arg_keys[1], (D,), jnp.float32), 0.1, 1.9)
    recept_weight = scatter_about(arg_keys[2], (D, HEADS * HEAD), D ** -0.5, 0.125, ((1, 2),))
    key_weight = scatter_about(arg_keys[3], (D, HEADS * HEAD), D ** -0.5, 0.125, ((1, 2),))
    value_weight = scatter_about(arg_keys[4], (D, HEADS * HEAD), D ** -0.5, 0.125, ((1, 2),))
    decay_down = scatter_about(arg_keys[5], (D, LOW), D ** -0.5, 0.125)
    decay_up = scatter_about(arg_keys[6], (LOW, HEADS * HEAD), LOW ** -0.5, 0.75)
    decay_bias = jnp.clip(jax.random.uniform(arg_keys[7], (HEADS * HEAD,), jnp.float32, -4.0, 1.0), -4.0, 1.0)
    rate_down = scatter_about(arg_keys[8], (D, LOW), D ** -0.5, 0.125)
    rate_up = scatter_about(arg_keys[9], (LOW, HEADS * HEAD), LOW ** -0.5, 0.75)
    rate_bias = scatter_about(arg_keys[10], (HEADS * HEAD,), 1.0, 4.0, (), jnp.float32)
    head_gain = jnp.clip(1.0 + 0.18 * jax.random.normal(arg_keys[11], (HEADS * HEAD,), jnp.float32), 0.1, 1.9)
    out_weight = scatter_about(arg_keys[12], (HEADS * HEAD, D), (HEADS * HEAD) ** -0.5, 0.1875, ((0, 2),))
    memory_state = scatter_about(arg_keys[13], (SEQUENCES, HEADS, HEAD, HEAD), 1.0, 6.0, ((0, 16), (1, 2)), jnp.float32)
    ffn_gain = jnp.clip(1.0 + 0.18 * jax.random.normal(arg_keys[14], (D,), jnp.float32), 0.1, 1.9)
    blend_vector = scatter_about(arg_keys[15], (D,), D ** -0.5, 0.125)
    dense_gate = scatter_about(arg_keys[16], (D, DFF), D ** -0.5, 0.125, ((1, 32),))
    dense_up = scatter_about(arg_keys[17], (D, DFF), D ** -0.5, 0.125, ((1, 32),))
    dense_down = scatter_about(arg_keys[18], (DFF, D), (DFF // 16) ** -0.5, 0.3125, ((0, 32),))
    expert_gate = scatter_about(arg_keys[19], (EXPERTS, D, EFF), D ** -0.5, 0.125, ((0, 16), (2, 2)))
    expert_up = scatter_about(arg_keys[20], (EXPERTS, D, EFF), D ** -0.5, 0.125, ((0, 16), (2, 2)))
    expert_down = scatter_about(arg_keys[21], (EXPERTS, EFF, D), EFF ** -0.5, 0.15625, ((0, 16), (1, 2)))
    routing_keys = jax.random.split(jax.random.fold_in(arg_keys[22], 1), SEQUENCES // SEQS)
    routing_turns = jax.random.permutation(jax.random.fold_in(arg_keys[22], 3), SEQUENCES // SEQS)
    routing = jax.vmap(lambda own, number: assign_block(jax.random.fold_in(arg_keys[22], 2), own, number, SEQS, EXPERTS, TOPK, CAP, 1))(routing_keys, routing_turns).reshape((SEQUENCES, TOPK))
    route_scale = jnp.clip(0.25 + 0.75 * jax.random.uniform(arg_keys[23], (SEQUENCES, TOPK), jnp.float32) ** block_scale(arg_keys[23], (SEQUENCES, TOPK), ((0, 16),), -0.2, 0.2), 0.25, 1.0)
    return {"hidden": hidden, "mix_gain": mix_gain, "recept_weight": recept_weight, "key_weight": key_weight, "value_weight": value_weight, "decay_down": decay_down, "decay_up": decay_up, "decay_bias": decay_bias, "rate_down": rate_down, "rate_up": rate_up, "rate_bias": rate_bias, "head_gain": head_gain, "out_weight": out_weight, "memory_state": memory_state, "ffn_gain": ffn_gain, "blend_vector": blend_vector, "dense_gate": dense_gate, "dense_up": dense_up, "dense_down": dense_down, "expert_gate": expert_gate, "expert_up": expert_up, "expert_down": expert_down, "routing": routing, "route_scale": route_scale}


def stored(tensor):
    return lax.optimization_barrier(tensor.astype(jnp.bfloat16)).astype(jnp.float32)

def rms_scaled(tensor, gain_vec):
    values = tensor.astype(jnp.float32)
    return values * lax.rsqrt(lax.optimization_barrier(jnp.mean(values * values, axis=-1, keepdims=True)) + 1e-06) * gain_vec

def silu_of(tensor):
    return tensor / (1.0 + jnp.exp(-tensor))

def matmul(left, right):
    return jnp.dot(left, right, preferred_element_type=jnp.float32)

def reference(hidden, mix_gain, recept_weight, key_weight, value_weight, decay_down, decay_up, decay_bias, rate_down, rate_up, rate_bias, head_gain, out_weight, memory_state, ffn_gain, blend_vector, dense_gate, dense_up, dense_down, expert_gate, expert_up, expert_down, routing, route_scale):
    seq_count = hidden.shape[0]
    full_width = HEADS * HEAD
    normed_in = rms_scaled(hidden, mix_gain).astype(jnp.bfloat16)
    recept_rows = stored(matmul(normed_in, recept_weight)).reshape(seq_count, HEADS, HEAD)
    key_rows = stored(matmul(normed_in, key_weight)).reshape(seq_count, HEADS, HEAD)
    value_rows = stored(matmul(normed_in, value_weight)).reshape(seq_count, HEADS, HEAD)
    decay_low = jnp.tanh(matmul(normed_in, decay_down)).astype(jnp.bfloat16)
    decay_pre = matmul(decay_low, decay_up) + decay_bias
    decay_rate = jnp.exp(-jnp.exp(-jax.nn.softplus(-decay_pre) - 0.5)).reshape(seq_count, HEADS, HEAD)
    rate_low = matmul(normed_in, rate_down).astype(jnp.bfloat16)
    learn_rate = jax.nn.sigmoid(matmul(rate_low, rate_up) + rate_bias).reshape(seq_count, HEADS, HEAD)
    unit_key = key_rows * lax.rsqrt(lax.optimization_barrier(jnp.sum(key_rows * key_rows, axis=-1, keepdims=True)) + 1e-06)
    removed = jnp.einsum('shij,shj->shi', memory_state, unit_key, precision=lax.Precision.HIGHEST)
    new_state = memory_state * decay_rate[:, :, None, :] - removed[..., None] * (unit_key * learn_rate)[:, :, None, :] + value_rows[..., None] * (key_rows * learn_rate)[:, :, None, :]
    readout = jnp.einsum('shij,shj->shi', new_state, recept_rows, precision=lax.Precision.HIGHEST)
    centre = lax.optimization_barrier(jnp.mean(readout, axis=-1, keepdims=True))
    variance = lax.optimization_barrier(jnp.mean(jnp.square(readout - centre), axis=-1, keepdims=True))
    head_normed = ((readout - centre) * lax.rsqrt(variance + 0.00064) * head_gain.reshape(HEADS, HEAD)).astype(jnp.bfloat16).reshape(seq_count, full_width)
    group_width = full_width // N_TP
    attn_sum = jnp.zeros((seq_count, D), jnp.float32)
    for group in range(N_TP):
        lower = group * group_width
        attn_sum = attn_sum + stored(matmul(head_normed[:, lower:lower + group_width], out_weight[lower:lower + group_width]))
    first_res = (hidden.astype(jnp.float32) + attn_sum).astype(jnp.bfloat16)
    ffn_in = rms_scaled(first_res, ffn_gain).astype(jnp.bfloat16)
    blend = jax.nn.sigmoid(jnp.dot(ffn_in, blend_vector, preferred_element_type=jnp.float32))
    dense_act = (silu_of(matmul(ffn_in, dense_gate)) * matmul(ffn_in, dense_up)).astype(jnp.bfloat16)
    dense_out = matmul(dense_act, dense_down)
    flat_route = routing.reshape(-1)
    flat_scale = route_scale.reshape(-1)
    slot_total = N_EP * CAP
    slot_index = jnp.arange(slot_total, dtype=jnp.int32)

    def one_expert(total, inputs):
        gate_mat, up_mat, down_mat, index = inputs
        chosen = flat_route == index
        live_count = jnp.sum(chosen.astype(jnp.int32))
        picks = jnp.nonzero(chosen, size=slot_total, fill_value=0)[0].astype(jnp.int32)
        owners = (picks // TOPK).astype(jnp.int32)
        rows = ffn_in[owners]
        live = slot_index < live_count
        scales = jnp.where(live, flat_scale[picks], jnp.zeros_like(flat_scale[picks]))
        expert_act = (silu_of(matmul(rows, gate_mat)) * matmul(rows, up_mat)).astype(jnp.bfloat16)
        expert_out = matmul(expert_act, down_mat)
        return (total.at[owners].add(expert_out * scales[:, None]), None)
    expert_sum, _ = lax.scan(one_expert, jnp.zeros((seq_count, D), jnp.float32), (expert_gate, expert_up, expert_down, jnp.arange(EXPERTS, dtype=jnp.int32)))
    layer_out = (first_res.astype(jnp.float32) + expert_sum + blend[:, None] * dense_out).astype(jnp.bfloat16)
    return (layer_out, new_state)
```

```python
import jax
import jax.numpy as jnp
from jax import lax
from jax.sharding import PartitionSpec as P


def stored(tensor):
    return lax.optimization_barrier(tensor.astype(jnp.bfloat16)).astype(jnp.float32)


def rms_scaled(tensor, gain_vec):
    values = tensor.astype(jnp.float32)
    return values * lax.rsqrt(jnp.mean(values * values, axis=-1, keepdims=True) + 1e-06) * gain_vec


def silu_of(tensor):
    return tensor / (1.0 + jnp.exp(-tensor))


def matmul(left, right):
    return jnp.dot(left, right, preferred_element_type=jnp.float32)


def grid_of(count):
    side = max(1, int(round((count / 4) ** 0.5)))
    if 4 * side * side == count:
        return (4, side, side)
    return (count, 1, 1)


def turned(index, dims, axis, step):
    place = [index // (dims[1] * dims[2]), index // dims[2] % dims[1], index % dims[2]]
    place[axis] = (place[axis] + step) % dims[axis]
    return (place[0] * dims[1] + place[1]) * dims[2] + place[2]


def hop(value, dims, axes, step):
    count = dims[0] * dims[1] * dims[2]
    perm = [
        (2 * chip + core, 2 * turned(chip, dims, axes[core], step) + core)
        for chip in range(count)
        for core in range(2)
    ]
    return lax.ppermute(value, ("ep", "tp"), perm)


def swap(value):
    return lax.ppermute(value, "tp", [(0, 1), (1, 0)])


ROUTES = ((0, 0), (2, 1), (1, 2))


def gather_tokens(rows, dims):
    held = rows
    for axes in ROUTES:
        size = dims[axes[0]]
        held = jnp.stack([held] + [hop(held, dims, axes, k) for k in range(1, size)], axis=-3)
    return held


def scatter_sums(sums, dims):
    for axes in reversed(ROUTES):
        size = dims[axes[0]]
        total = sums[..., 0, :, :].astype(jnp.float32)
        for k in range(1, size):
            total = total + hop(sums[..., k, :, :], dims, axes, -k).astype(jnp.float32)
        sums = total.astype(jnp.bfloat16) if axes[0] else total
    return sums


def shards(
    hidden,
    mix_gain,
    recept_weight,
    key_weight,
    value_weight,
    decay_down,
    decay_up,
    decay_bias,
    rate_down,
    rate_up,
    rate_bias,
    head_gain,
    out_weight,
    memory_state,
    ffn_gain,
    blend_vector,
    dense_gate,
    dense_up,
    dense_down,
    expert_gate,
    expert_up,
    expert_down,
    routing,
    route_scale,
):
    seq_count, model_width = hidden.shape
    own_width = recept_weight.shape[1]
    head_count = memory_state.shape[1]
    head_size = memory_state.shape[2]
    offset = lax.axis_index("tp") * own_width
    decay_up_own = lax.dynamic_slice_in_dim(decay_up, offset, own_width, 1)
    rate_up_own = lax.dynamic_slice_in_dim(rate_up, offset, own_width, 1)
    decay_bias_own = lax.dynamic_slice_in_dim(decay_bias, offset, own_width, 0)
    rate_bias_own = lax.dynamic_slice_in_dim(rate_bias, offset, own_width, 0)
    gain_own = lax.dynamic_slice_in_dim(head_gain, offset, own_width, 0)
    normed_in = rms_scaled(hidden, mix_gain).astype(jnp.bfloat16)
    split_shape = (seq_count, head_count, head_size)
    recept_rows = stored(matmul(normed_in, recept_weight)).reshape(split_shape)
    key_rows = stored(matmul(normed_in, key_weight)).reshape(split_shape)
    value_rows = stored(matmul(normed_in, value_weight)).reshape(split_shape)
    decay_low = jnp.tanh(matmul(normed_in, decay_down)).astype(jnp.bfloat16)
    decay_pre = matmul(decay_low, decay_up_own) + decay_bias_own
    decay_rate = jnp.exp(-jnp.exp(-jax.nn.softplus(-decay_pre) - 0.5)).reshape(split_shape)
    rate_low = matmul(normed_in, rate_down).astype(jnp.bfloat16)
    learn_rate = jax.nn.sigmoid(matmul(rate_low, rate_up_own) + rate_bias_own).reshape(split_shape)
    unit_key = key_rows * lax.rsqrt(jnp.sum(key_rows * key_rows, axis=-1, keepdims=True) + 1e-06)
    removed = jnp.einsum("shij,shj->shi", memory_state, unit_key, precision=lax.Precision.HIGHEST)
    new_state = (
        memory_state * decay_rate[:, :, None, :]
        - removed[..., None] * (unit_key * learn_rate)[:, :, None, :]
        + value_rows[..., None] * (key_rows * learn_rate)[:, :, None, :]
    )
    readout = jnp.einsum("shij,shj->shi", new_state, recept_rows, precision=lax.Precision.HIGHEST)
    centre = jnp.mean(readout, axis=-1, keepdims=True)
    variance = jnp.mean(jnp.square(readout - centre), axis=-1, keepdims=True)
    head_normed = (
        (
            (readout - centre)
            * lax.rsqrt(variance + 0.00064)
            * gain_own.reshape(head_count, head_size)
        )
        .astype(jnp.bfloat16)
        .reshape(seq_count, own_width)
    )
    core = lax.axis_index("tp")
    half_rows = seq_count // 2
    dims = grid_of(lax.axis_size("ep"))
    part = matmul(head_normed, out_weight).astype(jnp.bfloat16).reshape(2, half_rows, model_width)
    kept = lax.dynamic_index_in_dim(part, core, 0, keepdims=False)
    sent = lax.dynamic_index_in_dim(part, 1 - core, 0, keepdims=False)
    attn_sum = kept.astype(jnp.float32) + swap(sent).astype(jnp.float32)
    hidden_own = lax.dynamic_slice_in_dim(hidden, core * half_rows, half_rows, 0)
    first_res = (hidden_own.astype(jnp.float32) + attn_sum).astype(jnp.bfloat16)
    ffn_in = rms_scaled(first_res, ffn_gain).astype(jnp.bfloat16)

    chips = lax.axis_size("ep")
    top_count = routing.shape[1]
    slot_cap = max(2, 2 * seq_count * top_count // chips)
    notes = lax.dynamic_slice_in_dim(
        route_notes(routing, route_scale, chips), core * half_rows, half_rows, 0
    )
    rows = gather_tokens(jnp.concatenate([ffn_in, notes], axis=1), dims)
    other = swap(rows)
    lead = rows.shape[:3]
    ids = jnp.arange(chips, dtype=jnp.int32).reshape(lead)
    gate, scale = [], []
    pieces = []
    for value, numbers in ((rows, ids), (other, jnp.swapaxes(ids, 1, 2))):
        tokens = value[..., :model_width].reshape(-1, model_width)
        marks = value[..., model_width:].reshape(tokens.shape[0], -1).astype(jnp.float32)
        base = jnp.repeat(numbers.reshape(-1), half_rows) * slot_cap
        pieces.append((tokens, marks, base))
    tokens = jnp.concatenate([p[0] for p in pieces])
    marks = jnp.concatenate([p[1] for p in pieces])
    base = jnp.concatenate([p[2] for p in pieces])
    expert = lax.axis_index("ep").astype(jnp.float32)
    slot = jnp.full(base.shape, -1, jnp.int32)
    weight = jnp.zeros(base.shape, jnp.float32)
    for choice in range(top_count):
        named, rank, high, low = (marks[:, 4 * choice + k] for k in range(4))
        slot = jnp.where(named == expert, base + rank.astype(jnp.int32), slot)
        weight = jnp.where(named == expert, high + low, weight)
    chosen = jnp.arange(chips * slot_cap, dtype=jnp.int32)[:, None] == slot[None, :]
    slot_weight = jnp.sum(jnp.where(chosen, weight[None, :], 0.0), axis=1, keepdims=True)
    select = chosen.astype(jnp.bfloat16)
    picked = matmul(select, tokens).astype(jnp.bfloat16)
    expert_act = (silu_of(matmul(picked, expert_gate[0])) * matmul(picked, expert_up[0])).astype(
        jnp.bfloat16
    )
    expert_out = (matmul(expert_act, expert_down[0]) * slot_weight).astype(jnp.bfloat16)
    blend = jax.nn.sigmoid(jnp.dot(tokens, blend_vector, preferred_element_type=jnp.float32))
    dense_act = (
        silu_of(matmul(tokens, dense_gate)) * matmul(tokens, dense_up) * blend[:, None]
    ).astype(jnp.bfloat16)
    partial = lax.dot_general(
        select, expert_out, (((0,), (0,)), ((), ())), preferred_element_type=jnp.float32
    ) + matmul(dense_act, dense_down)
    partial = partial.reshape((2,) + lead + (half_rows, model_width)).astype(jnp.bfloat16)
    merged = (partial[0].astype(jnp.float32) + swap(partial[1]).astype(jnp.float32)).astype(
        jnp.bfloat16
    )
    mixed = scatter_sums(merged, dims)
    out_own = (first_res.astype(jnp.float32) + mixed).astype(jnp.bfloat16)
    out_other = swap(out_own)
    layer_out = jnp.concatenate(
        [jnp.where(core == 0, out_own, out_other), jnp.where(core == 0, out_other, out_own)]
    )
    return (layer_out, new_state)


def route_notes(routing, route_scale, chips):
    seq_count, top_count = routing.shape
    flat = routing.reshape(-1)
    one_hot = (flat[:, None] == jnp.arange(chips, dtype=jnp.int32)[None, :]).astype(jnp.int32)
    before = jnp.cumsum(one_hot, axis=0) - one_hot
    rank = jnp.sum(before * one_hot, axis=1).reshape(seq_count, top_count)
    high = route_scale.astype(jnp.bfloat16)
    low = (route_scale - high.astype(jnp.float32)).astype(jnp.bfloat16)
    fields = [routing.astype(jnp.bfloat16), rank.astype(jnp.bfloat16), high, low]
    notes = jnp.stack(fields, axis=2).reshape(seq_count, 4 * top_count)
    return jnp.pad(notes, ((0, 0), (0, 128 - 4 * top_count)))


def solution(mesh):
    in_specs = (
        P("ep", None),
        P(),
        P(None, "tp"),
        P(None, "tp"),
        P(None, "tp"),
        P(),
        P(),
        P(),
        P(),
        P(),
        P(),
        P(),
        P("tp", None),
        P("ep", "tp", None, None),
        P(),
        P(),
        P(None, ("ep", "tp")),
        P(None, ("ep", "tp")),
        P(("ep", "tp"), None),
        P("ep", None, "tp"),
        P("ep", None, "tp"),
        P("ep", "tp", None),
        P("ep", None),
        P("ep", None),
    )
    out_specs = (P("ep", None), P("ep", "tp", None, None))
    return jax.shard_map(shards, mesh=mesh, in_specs=in_specs, out_specs=out_specs, check_vma=False)
```

```python
import math

import jax
import jax.numpy as jnp
from jax import lax
from jax.experimental import pallas as pl
from jax.experimental.pallas import tpu as pltpu
from jax.sharding import PartitionSpec as P


def rms_scaled(tensor, gain_vec):
    values = tensor.astype(jnp.float32)
    return values * lax.rsqrt(jnp.mean(values * values, axis=-1, keepdims=True) + 1e-06) * gain_vec


def silu_of(tensor):
    return tensor / (1.0 + jnp.exp(-tensor))


def matmul(left, right):
    return jnp.dot(left, right, preferred_element_type=jnp.float32)


def grid_of(count):
    side = max(1, int(round((count / 4) ** 0.5)))
    if 4 * side * side == count:
        return (4, side, side)
    return (count, 1, 1)


def turned(index, dims, axis, step):
    place = [index // (dims[1] * dims[2]), index // dims[2] % dims[1], index % dims[2]]
    place[axis] = (place[axis] + step) % dims[axis]
    return (place[0] * dims[1] + place[1]) * dims[2] + place[2]


def hop(value, dims, axes, step):
    count = dims[0] * dims[1] * dims[2]
    perm = [
        (2 * chip + core, 2 * turned(chip, dims, axes[core], step) + core)
        for chip in range(count)
        for core in range(2)
    ]
    return lax.ppermute(value, ("ep", "tp"), perm)


def swap(value):
    return lax.ppermute(value, "tp", [(0, 1), (1, 0)])


ROUTES = ((0, 0), (2, 1), (1, 2))


def gather_tokens(rows, dims):
    held = rows
    for axes in ROUTES:
        size = dims[axes[0]]
        held = jnp.stack([held] + [hop(held, dims, axes, k) for k in range(1, size)], axis=-3)
    return held


def scatter_sums(sums, dims):
    for axes in reversed(ROUTES):
        size = dims[axes[0]]
        total = sums[..., 0, :, :].astype(jnp.float32)
        for k in range(1, size):
            total = total + hop(sums[..., k, :, :], dims, axes, -k).astype(jnp.float32)
        sums = total.astype(jnp.bfloat16) if axes[0] else total
    return sums


def attention_kernel(
    core_ref,
    hidden_ref,
    mix_ref,
    recept_ref,
    key_ref,
    value_ref,
    decay_down_ref,
    decay_up_ref,
    decay_bias_ref,
    rate_down_ref,
    rate_up_ref,
    rate_bias_ref,
    gain_ref,
    out_weight_ref,
    state_ref,
    part_ref,
    new_ref,
    unit_scr,
    pull_scr,
    push_scr,
    decay_scr,
    recept_scr,
    value_scr,
    head_scr,
):
    heads, seqs, size = unit_scr.shape
    block = state_ref.shape[0]
    step = pl.program_id(0)

    def flat_dot(left, right):
        return lax.dot_general(
            left, right, (((1,), (1,)), ((), ())), preferred_element_type=jnp.float32
        )

    @pl.when(step == 0)
    def _():
        normed = rms_scaled(hidden_ref[...], mix_ref[...]).astype(jnp.bfloat16)
        rounded = lambda value: value.astype(jnp.bfloat16).astype(jnp.float32)
        recept = rounded(matmul(normed, recept_ref[...]))
        key = rounded(matmul(normed, key_ref[...]))
        value = rounded(matmul(normed, value_ref[...]))
        decay_low = jnp.tanh(flat_dot(normed, decay_down_ref[...])).astype(jnp.bfloat16)
        decay_pre = matmul(decay_low, decay_up_ref[...]) + decay_bias_ref[...]
        decay = jnp.exp(-math.exp(-0.5) / (1.0 + jnp.exp(-decay_pre)))
        rate_low = flat_dot(normed, rate_down_ref[...]).astype(jnp.bfloat16)
        rate = 1.0 / (1.0 + jnp.exp(-(matmul(rate_low, rate_up_ref[...]) + rate_bias_ref[...])))
        for head in range(heads):
            cut = slice(head * size, (head + 1) * size)
            own_key = key[:, cut]
            unit = own_key * lax.rsqrt(
                jnp.sum(own_key * own_key, axis=-1, keepdims=True) + 1e-06
            )
            unit_scr[head] = unit
            pull_scr[head] = unit * rate[:, cut]
            push_scr[head] = own_key * rate[:, cut]
            decay_scr[head] = decay[:, cut]
            recept_scr[head] = recept[:, cut]
            value_scr[head] = value[:, cut]

    rows = pl.ds(pl.multiple_of(step * block, block), block)
    ones = jnp.ones((size, 128), jnp.bfloat16)
    lane = lax.broadcasted_iota(jnp.int32, (size, 128), 1)
    for head in range(heads):
        unit = unit_scr[head, rows, :]
        products = [
            (state_ref[seq, head] * unit[seq : seq + 1]).astype(jnp.bfloat16)
            for seq in range(block)
        ]
        removed = matmul(jnp.concatenate(products), ones)
        pull = pull_scr[head, rows, :]
        push = push_scr[head, rows, :]
        decay = decay_scr[head, rows, :]
        recept = recept_scr[head, rows, :]
        value = value_scr[head, rows, :].T
        products = []
        for seq in range(block):
            one = slice(seq, seq + 1)
            fresh = (
                state_ref[seq, head] * decay[one]
                - removed[seq * size : (seq + 1) * size, :size] * pull[one]
                + value[:, one] * push[one]
            )
            new_ref[seq, head] = fresh
            products.append((fresh * recept[one]).astype(jnp.bfloat16))
        readout = matmul(jnp.concatenate(products), ones)
        columns = jnp.zeros((size, 128), jnp.float32)
        for seq in range(block):
            columns = jnp.where(lane == seq, readout[seq * size : (seq + 1) * size], columns)
        lines = columns.T[:block]
        centred = lines - jnp.mean(lines, axis=-1, keepdims=True)
        variance = jnp.mean(centred * centred, axis=-1, keepdims=True)
        head_scr[head, rows, :] = (
            centred
            * lax.rsqrt(variance + 0.00064)
            * gain_ref[:, head * size : (head + 1) * size]
        )

    @pl.when(step == pl.num_programs(0) - 1)
    def _():
        lines = jnp.concatenate([head_scr[head] for head in range(heads)], axis=1)
        part_ref[...] = matmul(lines.astype(jnp.bfloat16), out_weight_ref[...]).astype(
            part_ref.dtype
        )


def attention(
    hidden,
    mix_gain,
    recept_weight,
    key_weight,
    value_weight,
    decay_down,
    decay_up,
    decay_bias,
    rate_down,
    rate_up,
    rate_bias,
    head_gain,
    out_weight,
    memory_state,
):
    seqs, width = hidden.shape
    _, heads, size, _ = memory_state.shape
    own = heads * size
    low = decay_down.shape[1]
    block = 8
    core = lax.axis_index("tp").astype(jnp.int32).reshape(1)
    whole = lambda *shape: pl.BlockSpec(shape, lambda i, c: (0,) * len(shape))
    half = lambda rows: pl.BlockSpec((rows, own), lambda i, c: (0, c[0]))
    state_spec = pl.BlockSpec((block, heads, size, size), lambda i, c: (i, 0, 0, 0))
    per_head = pltpu.VMEM((heads, seqs, size), jnp.float32)
    return pl.pallas_call(
        attention_kernel,
        grid_spec=pltpu.PrefetchScalarGridSpec(
            num_scalar_prefetch=1,
            grid=(seqs // block,),
            in_specs=[
                whole(seqs, width),
                whole(1, width),
                whole(width, own),
                whole(width, own),
                whole(width, own),
                whole(low, width),
                half(low),
                half(1),
                whole(low, width),
                half(low),
                half(1),
                half(1),
                whole(own, width),
                state_spec,
            ],
            out_specs=[whole(seqs, width), state_spec],
            scratch_shapes=[per_head] * 7,
        ),
        out_shape=[
            jax.ShapeDtypeStruct((seqs, width), jnp.bfloat16),
            jax.ShapeDtypeStruct(memory_state.shape, memory_state.dtype),
        ],
        compiler_params=pltpu.CompilerParams(
            dimension_semantics=("arbitrary",), vmem_limit_bytes=66000000
        ),
        name="attention",
    )(
        core,
        hidden,
        mix_gain[None],
        recept_weight,
        key_weight,
        value_weight,
        decay_down.T,
        decay_up,
        decay_bias[None],
        rate_down.T,
        rate_up,
        rate_bias[None],
        head_gain[None],
        out_weight,
        memory_state,
    )


def shards(
    hidden,
    mix_gain,
    recept_weight,
    key_weight,
    value_weight,
    decay_down,
    decay_up,
    decay_bias,
    rate_down,
    rate_up,
    rate_bias,
    head_gain,
    out_weight,
    memory_state,
    ffn_gain,
    blend_vector,
    dense_gate,
    dense_up,
    dense_down,
    expert_gate,
    expert_up,
    expert_down,
    routing,
    route_scale,
):
    seq_count, model_width = hidden.shape
    group_part, new_state = attention(
        hidden,
        mix_gain,
        recept_weight,
        key_weight,
        value_weight,
        decay_down,
        decay_up,
        decay_bias,
        rate_down,
        rate_up,
        rate_bias,
        head_gain,
        out_weight,
        memory_state,
    )
    core = lax.axis_index("tp")
    half_rows = seq_count // 2
    dims = grid_of(lax.axis_size("ep"))
    part = group_part.reshape(2, half_rows, model_width)
    kept = lax.dynamic_index_in_dim(part, core, 0, keepdims=False)
    sent = lax.dynamic_index_in_dim(part, 1 - core, 0, keepdims=False)
    attn_sum = kept.astype(jnp.float32) + swap(sent).astype(jnp.float32)
    hidden_own = lax.dynamic_slice_in_dim(hidden, core * half_rows, half_rows, 0)
    first_res = (hidden_own.astype(jnp.float32) + attn_sum).astype(jnp.bfloat16)
    ffn_in = rms_scaled(first_res, ffn_gain).astype(jnp.bfloat16)

    chips = lax.axis_size("ep")
    top_count = routing.shape[1]
    slot_cap = max(2, 2 * seq_count * top_count // chips)
    notes = lax.dynamic_slice_in_dim(
        route_notes(routing, route_scale, chips), core * half_rows, half_rows, 0
    )
    rows = gather_tokens(jnp.concatenate([ffn_in, notes], axis=1), dims)
    other = swap(rows)
    lead = rows.shape[:3]
    ids = jnp.arange(chips, dtype=jnp.int32).reshape(lead)
    gate, scale = [], []
    pieces = []
    for value, numbers in ((rows, ids), (other, jnp.swapaxes(ids, 1, 2))):
        tokens = value[..., :model_width].reshape(-1, model_width)
        marks = value[..., model_width:].reshape(tokens.shape[0], -1).astype(jnp.float32)
        base = jnp.repeat(numbers.reshape(-1), half_rows) * slot_cap
        pieces.append((tokens, marks, base))
    tokens = jnp.concatenate([p[0] for p in pieces])
    marks = jnp.concatenate([p[1] for p in pieces])
    base = jnp.concatenate([p[2] for p in pieces])
    expert = lax.axis_index("ep").astype(jnp.float32)
    slot = jnp.full(base.shape, -1, jnp.int32)
    weight = jnp.zeros(base.shape, jnp.float32)
    for choice in range(top_count):
        named, rank, high, low = (marks[:, 4 * choice + k] for k in range(4))
        slot = jnp.where(named == expert, base + rank.astype(jnp.int32), slot)
        weight = jnp.where(named == expert, high + low, weight)
    chosen = jnp.arange(chips * slot_cap, dtype=jnp.int32)[:, None] == slot[None, :]
    slot_weight = jnp.sum(jnp.where(chosen, weight[None, :], 0.0), axis=1, keepdims=True)
    select = chosen.astype(jnp.bfloat16)
    picked = matmul(select, tokens).astype(jnp.bfloat16)
    expert_act = (silu_of(matmul(picked, expert_gate[0])) * matmul(picked, expert_up[0])).astype(
        jnp.bfloat16
    )
    expert_out = (matmul(expert_act, expert_down[0]) * slot_weight).astype(jnp.bfloat16)
    blend = jax.nn.sigmoid(jnp.dot(tokens, blend_vector, preferred_element_type=jnp.float32))
    dense_act = (
        silu_of(matmul(tokens, dense_gate)) * matmul(tokens, dense_up) * blend[:, None]
    ).astype(jnp.bfloat16)
    partial = lax.dot_general(
        select, expert_out, (((0,), (0,)), ((), ())), preferred_element_type=jnp.float32
    ) + matmul(dense_act, dense_down)
    partial = partial.reshape((2,) + lead + (half_rows, model_width)).astype(jnp.bfloat16)
    merged = (partial[0].astype(jnp.float32) + swap(partial[1]).astype(jnp.float32)).astype(
        jnp.bfloat16
    )
    mixed = scatter_sums(merged, dims)
    out_own = (first_res.astype(jnp.float32) + mixed).astype(jnp.bfloat16)
    out_other = swap(out_own)
    layer_out = jnp.concatenate(
        [jnp.where(core == 0, out_own, out_other), jnp.where(core == 0, out_other, out_own)]
    )
    return (layer_out, new_state)


def route_notes(routing, route_scale, chips):
    seq_count, top_count = routing.shape
    flat = routing.reshape(-1)
    one_hot = (flat[:, None] == jnp.arange(chips, dtype=jnp.int32)[None, :]).astype(jnp.int32)
    before = jnp.cumsum(one_hot, axis=0) - one_hot
    rank = jnp.sum(before * one_hot, axis=1).reshape(seq_count, top_count)
    high = route_scale.astype(jnp.bfloat16)
    low = (route_scale - high.astype(jnp.float32)).astype(jnp.bfloat16)
    fields = [routing.astype(jnp.bfloat16), rank.astype(jnp.bfloat16), high, low]
    notes = jnp.stack(fields, axis=2).reshape(seq_count, 4 * top_count)
    return jnp.pad(notes, ((0, 0), (0, 128 - 4 * top_count)))


def solution(mesh):
    in_specs = (
        P("ep", None),
        P(),
        P(None, "tp"),
        P(None, "tp"),
        P(None, "tp"),
        P(),
        P(),
        P(),
        P(),
        P(),
        P(),
        P(),
        P("tp", None),
        P("ep", "tp", None, None),
        P(),
        P(),
        P(None, ("ep", "tp")),
        P(None, ("ep", "tp")),
        P(("ep", "tp"), None),
        P("ep", None, "tp"),
        P("ep", None, "tp"),
        P("ep", "tp", None),
        P("ep", None),
        P("ep", None),
    )
    out_specs = (P("ep", None), P("ep", "tp", None, None))
    return jax.shard_map(shards, mesh=mesh, in_specs=in_specs, out_specs=out_specs, check_vma=False)
```

```python
import functools
import math

import jax
import jax.numpy as jnp
from jax import lax
from jax.experimental import pallas as pl
from jax.experimental.pallas import tpu as pltpu
from jax.sharding import PartitionSpec as P


def rms_scaled(tensor, gain_vec):
    values = tensor.astype(jnp.float32)
    return values * lax.rsqrt(jnp.mean(values * values, axis=-1, keepdims=True) + 1e-06) * gain_vec


def silu_of(tensor):
    return tensor / (1.0 + jnp.exp(-tensor))


def matmul(left, right):
    return jnp.dot(left, right, preferred_element_type=jnp.float32)


def touch_kernel(*refs):
    refs[-1][0] = refs[0][0]


def touch(chip, *values):
    smem = pl.BlockSpec(memory_space=pltpu.SMEM)
    return pl.pallas_call(
        touch_kernel,
        in_specs=[smem] + [pl.BlockSpec(memory_space=pltpu.VMEM)] * len(values),
        out_specs=smem,
        out_shape=jax.ShapeDtypeStruct(chip.shape, chip.dtype),
        compiler_params=pltpu.CompilerParams(vmem_limit_bytes=12 * 1024 * 1024),
        name="touch",
    )(chip, *values)


def experts_kernel(
    pieces,
    cap,
    span,
    chip_ref,
    expert_gate_ref,
    expert_up_ref,
    expert_down_ref,
    dense_gate_ref,
    dense_up_ref,
    dense_down_ref,
    blend_ref,
    *refs,
):
    ins, outs = refs[: len(pieces)], refs[len(pieces) : 2 * len(pieces)]
    token_scr, act_scr = refs[2 * len(pieces) :]
    width = dense_down_ref.shape[-1]
    count, _ = ins[0].shape
    slots = len(pieces) // 2 * (count // span) * cap
    named = chip_ref[0].astype(jnp.float32)
    turn = lambda left, right: lax.dot_general(
        left, right, (((1,), (1,)), ((), ())), preferred_element_type=jnp.float32
    )
    row = lax.broadcasted_iota(jnp.int32, (count, 1), 0)
    lane = lax.broadcasted_iota(jnp.int32, (count, slots), 1)
    selects, weights = [], []
    for piece, ((scale_first, scale_rest, offset, inner), ref) in enumerate(zip(pieces, ins)):
        marks = ref[:, width:].astype(jnp.float32)
        block = row // span
        base = (block // inner) * scale_first + block % inner * scale_rest + offset
        slot = jnp.full((count, 1), -1, jnp.int32)
        weight = jnp.zeros((count, 1), jnp.float32)
        for choice in range(2):
            mark = lambda k: marks[:, 4 * choice + k : 4 * choice + k + 1]
            hit = mark(0) == named
            slot = jnp.where(hit, base * cap + mark(1).astype(jnp.int32), slot)
            weight = jnp.where(hit, mark(2) + mark(3), weight)
        selects.append(jnp.where(lane == slot, 1.0, 0.0).astype(jnp.bfloat16))
        weights.append(weight)
        token_scr[piece * count : (piece + 1) * count, :] = ref[:, :width]
    select = jnp.concatenate(selects)
    picked = lax.dot_general(
        select, token_scr[...], (((0,), (0,)), ((), ())), preferred_element_type=jnp.float32
    ).astype(jnp.bfloat16)
    tokens = token_scr[...]
    blend_rows = jnp.broadcast_to(blend_ref[...], (8, width))
    blend = 1.0 / (1.0 + jnp.exp(-turn(tokens, blend_rows)[:, :1]))
    act_scr[...] = (
        silu_of(turn(tokens, dense_gate_ref[...])) * turn(tokens, dense_up_ref[...]) * blend
    ).astype(jnp.bfloat16)
    gate = silu_of(matmul(picked, expert_gate_ref[0]))
    expert_act = (gate * matmul(picked, expert_up_ref[0])).astype(jnp.bfloat16)
    expert_out = matmul(expert_act, expert_down_ref[0]).astype(jnp.bfloat16)
    for piece in range(len(pieces)):
        outs[piece][...] = (
            matmul(selects[piece], expert_out) * weights[piece]
            + matmul(act_scr[piece * count : (piece + 1) * count, :], dense_down_ref[...])
        ).astype(jnp.bfloat16)


def experts(own, other, cap, span, chip, weights):
    sides, (firsts, group, _, wide) = len(own), own[0].shape
    count = firsts * group * span
    flat = [value.reshape(count, wide) for value in own + other]
    pieces = [(group, 1, s * firsts * group, group) for s in range(sides)]
    pieces += [(firsts * group, 1, s * group, group) for s in range(sides)]
    width = weights[2].shape[-1]
    vmem = pl.BlockSpec(memory_space=pltpu.VMEM)
    units = weights[0].shape[-1]
    rows = 2 * sides * count
    outs = pl.pallas_call(
        functools.partial(experts_kernel, tuple(pieces), cap, span),
        in_specs=[pl.BlockSpec(memory_space=pltpu.SMEM)] + [vmem] * (len(weights) + len(flat)),
        out_specs=[vmem] * len(flat),
        out_shape=[jax.ShapeDtypeStruct((count, width), jnp.bfloat16)] * len(flat),
        scratch_shapes=[
            pltpu.VMEM((rows, width), jnp.bfloat16),
            pltpu.VMEM((rows, weights[3].shape[0]), jnp.bfloat16),
        ],
        compiler_params=pltpu.CompilerParams(vmem_limit_bytes=16 * 1024 * 1024 + rows * 24000),
        cost_estimate=pl.CostEstimate(
            flops=6 * rows * width * 2 * units, bytes_accessed=6 * width * units, transcendentals=0
        ),
        name="experts",
    )(chip, *weights, *flat)
    outs = [value.reshape(firsts, group, span, width) for value in outs]
    return outs[:sides], outs[sides:]


def grid_of(count):
    side = max(1, int(round((count / 4) ** 0.5)))
    if 4 * side * side == count:
        return (4, side, side)
    return (count, 1, 1)


def turned(index, dims, axis, step):
    place = [index // (dims[1] * dims[2]), index // dims[2] % dims[1], index % dims[2]]
    place[axis] = (place[axis] + step) % dims[axis]
    return (place[0] * dims[1] + place[1]) * dims[2] + place[2]


def hop(value, dims, axes, step):
    count = dims[0] * dims[1] * dims[2]
    perm = [
        (2 * chip + core, 2 * turned(chip, dims, axes[core], step) + core)
        for chip in range(count)
        for core in range(2)
    ]
    return lax.ppermute(value, ("ep", "tp"), perm)


def swap(value):
    return lax.ppermute(value, "tp", [(0, 1), (1, 0)])


LINE, FIRST, SECOND = (0, 0), (2, 1), (1, 2)


def total(*values):
    return sum(value.astype(jnp.float32) for value in values).astype(jnp.bfloat16)


def plane_gather(blocks, dims):
    near = range(1, dims[1])
    firsts = jnp.stack([blocks] + [hop(blocks, dims, FIRST, k) for k in near])
    own = [firsts] + [hop(firsts, dims, SECOND, k) for k in near]
    other = [swap(own[0])]
    return own, other + [swap(value) for value in own[1:]]


def plane_reduce(own, other, dims):
    near = range(1, dims[1])
    back = [swap(other[k]) for k in near]
    back = [swap(other[0])] + back
    arrived = [hop(total(own[k], back[k]), dims, SECOND, -k) for k in near]
    firsts = total(own[0], back[0], *arrived)
    return total(firsts[0], *[hop(firsts[k], dims, FIRST, -k) for k in near])


def attention_kernel(
    core_ref,
    hidden_ref,
    mix_ref,
    recept_ref,
    key_ref,
    value_ref,
    decay_down_ref,
    decay_up_ref,
    decay_bias_ref,
    rate_down_ref,
    rate_up_ref,
    rate_bias_ref,
    gain_ref,
    out_weight_ref,
    state_ref,
    kept_ref,
    sent_ref,
    new_ref,
    unit_scr,
    pull_scr,
    push_scr,
    decay_scr,
    recept_scr,
    value_scr,
    head_scr,
):
    heads, seqs, size = unit_scr.shape
    block = state_ref.shape[0]
    step = pl.program_id(0)

    def flat_dot(left, right):
        return lax.dot_general(
            left, right, (((1,), (1,)), ((), ())), preferred_element_type=jnp.float32
        )

    @pl.when(step == 0)
    def _():
        normed = rms_scaled(hidden_ref[...], mix_ref[...]).astype(jnp.bfloat16)
        rounded = lambda value: value.astype(jnp.bfloat16).astype(jnp.float32)
        recept = rounded(matmul(normed, recept_ref[...]))
        key = rounded(matmul(normed, key_ref[...]))
        value = rounded(matmul(normed, value_ref[...]))
        decay_low = jnp.tanh(flat_dot(normed, decay_down_ref[...])).astype(jnp.bfloat16)
        decay_pre = matmul(decay_low, decay_up_ref[...]) + decay_bias_ref[...]
        decay = jnp.exp(-math.exp(-0.5) / (1.0 + jnp.exp(-decay_pre)))
        rate_low = flat_dot(normed, rate_down_ref[...]).astype(jnp.bfloat16)
        rate = 1.0 / (1.0 + jnp.exp(-(matmul(rate_low, rate_up_ref[...]) + rate_bias_ref[...])))
        for head in range(heads):
            cut = slice(head * size, (head + 1) * size)
            own_key = key[:, cut]
            unit = own_key * lax.rsqrt(
                jnp.sum(own_key * own_key, axis=-1, keepdims=True) + 1e-06
            )
            unit_scr[head] = unit
            pull_scr[head] = unit * rate[:, cut]
            push_scr[head] = own_key * rate[:, cut]
            decay_scr[head] = decay[:, cut]
            recept_scr[head] = recept[:, cut]
            value_scr[head] = value[:, cut]

    rows = pl.ds(pl.multiple_of(step * block, block), block)
    ones = jnp.ones((size, 128), jnp.bfloat16)
    lane = lax.broadcasted_iota(jnp.int32, (size, 128), 1)
    for head in range(heads):
        unit = unit_scr[head, rows, :]
        products = [
            (state_ref[seq, head] * unit[seq : seq + 1]).astype(jnp.bfloat16)
            for seq in range(block)
        ]
        removed = matmul(jnp.concatenate(products), ones)
        pull = pull_scr[head, rows, :]
        push = push_scr[head, rows, :]
        decay = decay_scr[head, rows, :]
        recept = recept_scr[head, rows, :]
        value = value_scr[head, rows, :].T
        products = []
        for seq in range(block):
            one = slice(seq, seq + 1)
            fresh = (
                state_ref[seq, head] * decay[one]
                - removed[seq * size : (seq + 1) * size, :size] * pull[one]
                + value[:, one] * push[one]
            )
            new_ref[seq, head] = fresh
            products.append((fresh * recept[one]).astype(jnp.bfloat16))
        readout = matmul(jnp.concatenate(products), ones)
        columns = jnp.zeros((size, 128), jnp.float32)
        for seq in range(block):
            columns = jnp.where(lane == seq, readout[seq * size : (seq + 1) * size], columns)
        lines = columns.T[:block]
        centred = lines - jnp.mean(lines, axis=-1, keepdims=True)
        variance = jnp.mean(centred * centred, axis=-1, keepdims=True)
        head_scr[head, rows, :] = (
            centred
            * lax.rsqrt(variance + 0.00064)
            * gain_ref[:, head * size : (head + 1) * size]
        )

    @pl.when(step == pl.num_programs(0) - 1)
    def _():
        half = seqs // 2
        for side, ref in ((core_ref[0], kept_ref), (1 - core_ref[0], sent_ref)):
            picked = pl.ds(pl.multiple_of(side * half, half), half)
            lines = jnp.concatenate([head_scr[head, picked, :] for head in range(heads)], axis=1)
            ref[...] = matmul(lines.astype(jnp.bfloat16), out_weight_ref[...]).astype(ref.dtype)


def attention(
    hidden,
    mix_gain,
    recept_weight,
    key_weight,
    value_weight,
    decay_down,
    decay_up,
    decay_bias,
    rate_down,
    rate_up,
    rate_bias,
    head_gain,
    out_weight,
    memory_state,
):
    seqs, width = hidden.shape
    _, heads, size, _ = memory_state.shape
    own = heads * size
    low = decay_down.shape[1]
    block = 8
    core = lax.axis_index("tp").astype(jnp.int32).reshape(1)
    whole = lambda *shape: pl.BlockSpec(shape, lambda i, c: (0,) * len(shape))
    half = lambda rows: pl.BlockSpec((rows, own), lambda i, c: (0, c[0]))
    state_spec = pl.BlockSpec((block, heads, size, size), lambda i, c: (i, 0, 0, 0))
    per_head = pltpu.VMEM((heads, seqs, size), jnp.float32)
    return pl.pallas_call(
        attention_kernel,
        grid_spec=pltpu.PrefetchScalarGridSpec(
            num_scalar_prefetch=1,
            grid=(seqs // block,),
            in_specs=[
                whole(seqs, width),
                whole(1, width),
                whole(width, own),
                whole(width, own),
                whole(width, own),
                whole(low, width),
                half(low),
                half(1),
                whole(low, width),
                half(low),
                half(1),
                half(1),
                whole(own, width),
                state_spec,
            ],
            out_specs=[whole(seqs // 2, width), whole(seqs // 2, width), state_spec],
            scratch_shapes=[per_head] * 7,
        ),
        out_shape=[
            jax.ShapeDtypeStruct((seqs // 2, width), jnp.bfloat16),
            jax.ShapeDtypeStruct((seqs // 2, width), jnp.bfloat16),
            jax.ShapeDtypeStruct(memory_state.shape, memory_state.dtype),
        ],
        compiler_params=pltpu.CompilerParams(
            dimension_semantics=("arbitrary",), vmem_limit_bytes=66000000
        ),
        name="attention",
    )(
        core,
        hidden,
        mix_gain[None],
        recept_weight,
        key_weight,
        value_weight,
        decay_down.T,
        decay_up,
        decay_bias[None],
        rate_down.T,
        rate_up,
        rate_bias[None],
        head_gain[None],
        out_weight,
        memory_state,
    )


def shards(
    hidden,
    mix_gain,
    recept_weight,
    key_weight,
    value_weight,
    decay_down,
    decay_up,
    decay_bias,
    rate_down,
    rate_up,
    rate_bias,
    head_gain,
    out_weight,
    memory_state,
    ffn_gain,
    blend_vector,
    dense_gate,
    dense_up,
    dense_down,
    expert_gate,
    expert_up,
    expert_down,
    routing,
    route_scale,
):
    seq_count, _ = hidden.shape
    kept, sent, new_state = attention(
        hidden,
        mix_gain,
        recept_weight,
        key_weight,
        value_weight,
        decay_down,
        decay_up,
        decay_bias,
        rate_down,
        rate_up,
        rate_bias,
        head_gain,
        out_weight,
        memory_state,
    )
    core = lax.axis_index("tp")
    half_rows = seq_count // 2
    chips = lax.axis_size("ep")
    dims = grid_of(chips)
    top_count = routing.shape[1]
    slot_cap = max(2, 2 * seq_count * top_count // chips)
    attn_sum = kept.astype(jnp.float32) + swap(sent).astype(jnp.float32)
    hidden_own = lax.dynamic_slice_in_dim(hidden, core * half_rows, half_rows, 0)
    first_res = (hidden_own.astype(jnp.float32) + attn_sum).astype(jnp.bfloat16)
    ffn_in = rms_scaled(first_res, ffn_gain).astype(jnp.bfloat16)
    notes = lax.dynamic_slice_in_dim(
        route_notes(routing, route_scale, chips), core * half_rows, half_rows, 0
    )
    rows = jnp.concatenate([ffn_in, notes], axis=1)

    near = dims[0] // 2
    line = [rows] + [hop(rows, dims, LINE, k) for k in range(1, dims[0])]
    chip = lax.axis_index("ep").astype(jnp.int32).reshape(1)
    weights = (
        expert_gate,
        expert_up,
        expert_down,
        dense_gate.T,
        dense_up.T,
        dense_down,
        blend_vector[None],
    )
    chip = touch(chip, *weights[:2])
    chip = touch(chip, *weights[2:6])
    sums = [first_res]
    for start in (0, near):
        own, other = plane_gather(jnp.stack(line[start : start + near]), dims)
        own, other = experts(own, other, slot_cap, half_rows, chip, weights)
        reduced = plane_reduce(own, other, dims)
        for k in range(near):
            if start + k:
                sums.append(hop(reduced[k], dims, LINE, -start - k))
            else:
                sums.append(reduced[k])
    out_own = total(*sums)
    out_other = swap(out_own)
    layer_out = jnp.concatenate(
        [jnp.where(core == 0, out_own, out_other), jnp.where(core == 0, out_other, out_own)]
    )
    return (layer_out, new_state)


def route_notes(routing, route_scale, chips):
    seq_count, top_count = routing.shape
    flat = routing.reshape(-1)
    one_hot = (flat[:, None] == jnp.arange(chips, dtype=jnp.int32)[None, :]).astype(jnp.int32)
    before = jnp.cumsum(one_hot, axis=0) - one_hot
    rank = jnp.sum(before * one_hot, axis=1).reshape(seq_count, top_count)
    high = route_scale.astype(jnp.bfloat16)
    low = (route_scale - high.astype(jnp.float32)).astype(jnp.bfloat16)
    fields = [routing.astype(jnp.bfloat16), rank.astype(jnp.bfloat16), high, low]
    notes = jnp.stack(fields, axis=2).reshape(seq_count, 4 * top_count)
    return jnp.pad(notes, ((0, 0), (0, 128 - 4 * top_count)))


def solution(mesh):
    in_specs = (
        P("ep", None),
        P(),
        P(None, "tp"),
        P(None, "tp"),
        P(None, "tp"),
        P(),
        P(),
        P(),
        P(),
        P(),
        P(),
        P(),
        P("tp", None),
        P("ep", "tp", None, None),
        P(),
        P(),
        P(None, ("ep", "tp")),
        P(None, ("ep", "tp")),
        P(("ep", "tp"), None),
        P("ep", None, "tp"),
        P("ep", None, "tp"),
        P("ep", "tp", None),
        P("ep", None),
        P("ep", None),
    )
    out_specs = (P("ep", None), P("ep", "tp", None, None))

    return jax.shard_map(shards, mesh=mesh, in_specs=in_specs, out_specs=out_specs, check_vma=False)
```

```python
import functools
import math

import jax
import jax.numpy as jnp
from jax import lax
from jax.experimental import pallas as pl
from jax.experimental.pallas import tpu as pltpu
from jax.sharding import PartitionSpec as P


def rms_scaled(tensor, gain_vec):
    values = tensor.astype(jnp.float32)
    return values * lax.rsqrt(jnp.mean(values * values, axis=-1, keepdims=True) + 1e-06) * gain_vec


def silu_of(tensor):
    return tensor / (1.0 + jnp.exp(-tensor))


def matmul(left, right):
    return jnp.dot(left, right, preferred_element_type=jnp.float32)


def touch_kernel(*refs):
    refs[-1][0] = refs[0][0]


def touch(chip, *values):
    smem = pl.BlockSpec(memory_space=pltpu.SMEM)
    return pl.pallas_call(
        touch_kernel,
        in_specs=[smem] + [pl.BlockSpec(memory_space=pltpu.VMEM)] * len(values),
        out_specs=smem,
        out_shape=jax.ShapeDtypeStruct(chip.shape, chip.dtype),
        compiler_params=pltpu.CompilerParams(vmem_limit_bytes=12 * 1024 * 1024),
        name="touch",
    )(chip, *values)


def experts_kernel(
    pieces,
    cap,
    span,
    chip_ref,
    expert_gate_ref,
    expert_up_ref,
    expert_down_ref,
    dense_gate_ref,
    dense_up_ref,
    dense_down_ref,
    blend_ref,
    *refs,
):
    ins, outs = refs[: len(pieces)], refs[len(pieces) : 2 * len(pieces)]
    token_scr, act_scr = refs[2 * len(pieces) :]
    width = dense_down_ref.shape[-1]
    count, _ = ins[0].shape
    slots = len(pieces) // 2 * (count // span) * cap
    named = chip_ref[0].astype(jnp.float32)
    turn = lambda left, right: lax.dot_general(
        left, right, (((1,), (1,)), ((), ())), preferred_element_type=jnp.float32
    )
    row = lax.broadcasted_iota(jnp.int32, (count, 1), 0)
    lane = lax.broadcasted_iota(jnp.int32, (count, slots), 1)
    selects, weights = [], []
    for piece, ((scale_first, scale_rest, offset, inner), ref) in enumerate(zip(pieces, ins)):
        marks = ref[:, width:].astype(jnp.float32)
        block = row // span
        base = (block // inner) * scale_first + block % inner * scale_rest + offset
        slot = jnp.full((count, 1), -1, jnp.int32)
        weight = jnp.zeros((count, 1), jnp.float32)
        for choice in range(2):
            mark = lambda k: marks[:, 4 * choice + k : 4 * choice + k + 1]
            hit = mark(0) == named
            slot = jnp.where(hit, base * cap + mark(1).astype(jnp.int32), slot)
            weight = jnp.where(hit, mark(2) + mark(3), weight)
        selects.append(jnp.where(lane == slot, 1.0, 0.0).astype(jnp.bfloat16))
        weights.append(weight)
        token_scr[piece * count : (piece + 1) * count, :] = ref[:, :width]
    select = jnp.concatenate(selects)
    picked = lax.dot_general(
        select, token_scr[...], (((0,), (0,)), ((), ())), preferred_element_type=jnp.float32
    ).astype(jnp.bfloat16)
    tokens = token_scr[...]
    blend_rows = jnp.broadcast_to(blend_ref[...], (8, width))
    blend = 1.0 / (1.0 + jnp.exp(-turn(tokens, blend_rows)[:, :1]))
    act_scr[...] = (
        silu_of(turn(tokens, dense_gate_ref[...])) * turn(tokens, dense_up_ref[...]) * blend
    ).astype(jnp.bfloat16)
    gate = silu_of(matmul(picked, expert_gate_ref[0]))
    expert_act = (gate * matmul(picked, expert_up_ref[0])).astype(jnp.bfloat16)
    expert_out = matmul(expert_act, expert_down_ref[0]).astype(jnp.bfloat16)
    for piece in range(len(pieces)):
        outs[piece][...] = (
            matmul(selects[piece], expert_out) * weights[piece]
            + matmul(act_scr[piece * count : (piece + 1) * count, :], dense_down_ref[...])
        ).astype(jnp.bfloat16)


def experts(own, other, cap, span, chip, weights):
    sides, (firsts, group, _, wide) = len(own), own[0].shape
    count = firsts * group * span
    flat = [value.reshape(count, wide) for value in own + other]
    pieces = [(group, 1, s * firsts * group, group) for s in range(sides)]
    pieces += [(firsts * group, 1, s * group, group) for s in range(sides)]
    width = weights[2].shape[-1]
    vmem = pl.BlockSpec(memory_space=pltpu.VMEM)
    units = weights[0].shape[-1]
    rows = 2 * sides * count
    outs = pl.pallas_call(
        functools.partial(experts_kernel, tuple(pieces), cap, span),
        in_specs=[pl.BlockSpec(memory_space=pltpu.SMEM)] + [vmem] * (len(weights) + len(flat)),
        out_specs=[vmem] * len(flat),
        out_shape=[jax.ShapeDtypeStruct((count, width), jnp.bfloat16)] * len(flat),
        scratch_shapes=[
            pltpu.VMEM((rows, width), jnp.bfloat16),
            pltpu.VMEM((rows, weights[3].shape[0]), jnp.bfloat16),
        ],
        compiler_params=pltpu.CompilerParams(vmem_limit_bytes=16 * 1024 * 1024 + rows * 24000),
        cost_estimate=pl.CostEstimate(
            flops=6 * rows * width * 2 * units, bytes_accessed=6 * width * units, transcendentals=0
        ),
        name="experts",
    )(chip, *weights, *flat)
    outs = [value.reshape(firsts, group, span, width) for value in outs]
    return outs[:sides], outs[sides:]


def grid_of(count):
    side = max(1, int(round((count / 4) ** 0.5)))
    if 4 * side * side == count:
        return (4, side, side)
    return (count, 1, 1)


def turned(index, dims, axis, step):
    place = [index // (dims[1] * dims[2]), index // dims[2] % dims[1], index % dims[2]]
    place[axis] = (place[axis] + step) % dims[axis]
    return (place[0] * dims[1] + place[1]) * dims[2] + place[2]


def hop(value, dims, axes, step):
    count = dims[0] * dims[1] * dims[2]
    perm = [
        (2 * chip + core, 2 * turned(chip, dims, axes[core], step) + core)
        for chip in range(count)
        for core in range(2)
    ]
    return lax.ppermute(value, ("ep", "tp"), perm)


def swap(value):
    return lax.ppermute(value, "tp", [(0, 1), (1, 0)])


LINE, FIRST, SECOND = (0, 0), (2, 1), (1, 2)


def total(*values):
    return sum(value.astype(jnp.float32) for value in values).astype(jnp.bfloat16)


def plane_gather(blocks, dims):
    near = range(1, dims[1])
    firsts = jnp.stack([blocks] + [hop(blocks, dims, FIRST, k) for k in near])
    own = [firsts] + [hop(firsts, dims, SECOND, k) for k in near]
    other = [swap(own[0])]
    return own, other + [swap(value) for value in own[1:]]


def plane_reduce(own, other, dims):
    near = range(1, dims[1])
    back = [swap(other[k]) for k in near]
    back = [swap(other[0])] + back
    arrived = [hop(total(own[k], back[k]), dims, SECOND, -k) for k in near]
    firsts = total(own[0], back[0], *arrived)
    return total(firsts[0], *[hop(firsts[k], dims, FIRST, -k) for k in near])


def attention_kernel(
    core_ref,
    hidden_ref,
    mix_ref,
    recept_ref,
    key_ref,
    value_ref,
    decay_down_ref,
    decay_up_ref,
    decay_bias_ref,
    rate_down_ref,
    rate_up_ref,
    rate_bias_ref,
    gain_ref,
    out_weight_ref,
    state_ref,
    kept_ref,
    sent_ref,
    new_ref,
    unit_scr,
    pull_scr,
    push_scr,
    decay_scr,
    recept_scr,
    value_scr,
    head_scr,
):
    heads, seqs, size = unit_scr.shape
    block = state_ref.shape[0]
    step = pl.program_id(0)

    def flat_dot(left, right):
        return lax.dot_general(
            left, right, (((1,), (1,)), ((), ())), preferred_element_type=jnp.float32
        )

    @pl.when(step == 0)
    def _():
        normed = rms_scaled(hidden_ref[...], mix_ref[...]).astype(jnp.bfloat16)
        rounded = lambda value: value.astype(jnp.bfloat16).astype(jnp.float32)
        recept = rounded(matmul(normed, recept_ref[...]))
        key = rounded(matmul(normed, key_ref[...]))
        value = rounded(matmul(normed, value_ref[...]))
        decay_low = jnp.tanh(flat_dot(normed, decay_down_ref[...])).astype(jnp.bfloat16)
        decay_pre = matmul(decay_low, decay_up_ref[...]) + decay_bias_ref[...]
        decay = jnp.exp(-math.exp(-0.5) / (1.0 + jnp.exp(-decay_pre)))
        rate_low = flat_dot(normed, rate_down_ref[...]).astype(jnp.bfloat16)
        rate = 1.0 / (1.0 + jnp.exp(-(matmul(rate_low, rate_up_ref[...]) + rate_bias_ref[...])))
        for head in range(heads):
            cut = slice(head * size, (head + 1) * size)
            own_key = key[:, cut]
            unit = own_key * lax.rsqrt(
                jnp.sum(own_key * own_key, axis=-1, keepdims=True) + 1e-06
            )
            unit_scr[head] = unit
            pull_scr[head] = unit * rate[:, cut]
            push_scr[head] = own_key * rate[:, cut]
            decay_scr[head] = decay[:, cut]
            recept_scr[head] = recept[:, cut]
            value_scr[head] = value[:, cut]

    rows = pl.ds(pl.multiple_of(step * block, block), block)
    ones = jnp.ones((size, 128), jnp.bfloat16)
    lane = lax.broadcasted_iota(jnp.int32, (size, 128), 1)

    def pulled(head):
        unit = unit_scr[head, rows, :]
        products = [
            (state_ref[seq, head] * unit[seq : seq + 1]).astype(jnp.bfloat16)
            for seq in range(block)
        ]
        return matmul(jnp.concatenate(products), ones)

    def updated(head, removed):
        pull = pull_scr[head, rows, :]
        push = push_scr[head, rows, :]
        decay = decay_scr[head, rows, :]
        recept = recept_scr[head, rows, :]
        value = value_scr[head, rows, :].T
        products = []
        for seq in range(block):
            one = slice(seq, seq + 1)
            fresh = (
                state_ref[seq, head] * decay[one]
                - removed[seq * size : (seq + 1) * size, :size] * pull[one]
                + value[:, one] * push[one]
            )
            new_ref[seq, head] = fresh
            products.append((fresh * recept[one]).astype(jnp.bfloat16))
        return matmul(jnp.concatenate(products), ones)

    def normed(head, readout):
        columns = jnp.zeros((size, 128), jnp.float32)
        for seq in range(block):
            columns = jnp.where(lane == seq, readout[seq * size : (seq + 1) * size], columns)
        lines = columns.T[:block]
        centred = lines - jnp.mean(lines, axis=-1, keepdims=True)
        variance = jnp.mean(centred * centred, axis=-1, keepdims=True)
        head_scr[head, rows, :] = (
            centred
            * lax.rsqrt(variance + 0.00064)
            * gain_ref[:, head * size : (head + 1) * size]
        )

    removed = pulled(0)
    readout = None
    for head in range(heads):
        following = pulled(head + 1) if head + 1 < heads else None
        finished = updated(head, removed)
        if head:
            normed(head - 1, readout)
        removed, readout = following, finished
    normed(heads - 1, readout)

    @pl.when(step == pl.num_programs(0) - 1)
    def _():
        half = seqs // 2
        for side, ref in ((core_ref[0], kept_ref), (1 - core_ref[0], sent_ref)):
            picked = pl.ds(pl.multiple_of(side * half, half), half)
            lines = jnp.concatenate([head_scr[head, picked, :] for head in range(heads)], axis=1)
            ref[...] = matmul(lines.astype(jnp.bfloat16), out_weight_ref[...]).astype(ref.dtype)


def attention(
    hidden,
    mix_gain,
    recept_weight,
    key_weight,
    value_weight,
    decay_down,
    decay_up,
    decay_bias,
    rate_down,
    rate_up,
    rate_bias,
    head_gain,
    out_weight,
    memory_state,
):
    seqs, width = hidden.shape
    _, heads, size, _ = memory_state.shape
    own = heads * size
    low = decay_down.shape[1]
    block = 8
    core = lax.axis_index("tp").astype(jnp.int32).reshape(1)
    whole = lambda *shape: pl.BlockSpec(shape, lambda i, c: (0,) * len(shape))
    half = lambda rows: pl.BlockSpec((rows, own), lambda i, c: (0, c[0]))
    state_spec = pl.BlockSpec((block, heads, size, size), lambda i, c: (i, 0, 0, 0))
    per_head = pltpu.VMEM((heads, seqs, size), jnp.float32)
    return pl.pallas_call(
        attention_kernel,
        grid_spec=pltpu.PrefetchScalarGridSpec(
            num_scalar_prefetch=1,
            grid=(seqs // block,),
            in_specs=[
                whole(seqs, width),
                whole(1, width),
                whole(width, own),
                whole(width, own),
                whole(width, own),
                whole(low, width),
                half(low),
                half(1),
                whole(low, width),
                half(low),
                half(1),
                half(1),
                whole(own, width),
                state_spec,
            ],
            out_specs=[whole(seqs // 2, width), whole(seqs // 2, width), state_spec],
            scratch_shapes=[per_head] * 7,
        ),
        out_shape=[
            jax.ShapeDtypeStruct((seqs // 2, width), jnp.bfloat16),
            jax.ShapeDtypeStruct((seqs // 2, width), jnp.bfloat16),
            jax.ShapeDtypeStruct(memory_state.shape, memory_state.dtype),
        ],
        compiler_params=pltpu.CompilerParams(
            dimension_semantics=("arbitrary",), vmem_limit_bytes=66000000
        ),
        name="attention",
    )(
        core,
        hidden,
        mix_gain[None],
        recept_weight,
        key_weight,
        value_weight,
        decay_down.T,
        decay_up,
        decay_bias[None],
        rate_down.T,
        rate_up,
        rate_bias[None],
        head_gain[None],
        out_weight,
        memory_state,
    )


def shards(
    hidden,
    mix_gain,
    recept_weight,
    key_weight,
    value_weight,
    decay_down,
    decay_up,
    decay_bias,
    rate_down,
    rate_up,
    rate_bias,
    head_gain,
    out_weight,
    memory_state,
    ffn_gain,
    blend_vector,
    dense_gate,
    dense_up,
    dense_down,
    expert_gate,
    expert_up,
    expert_down,
    routing,
    route_scale,
):
    seq_count, _ = hidden.shape
    kept, sent, new_state = attention(
        hidden,
        mix_gain,
        recept_weight,
        key_weight,
        value_weight,
        decay_down,
        decay_up,
        decay_bias,
        rate_down,
        rate_up,
        rate_bias,
        head_gain,
        out_weight,
        memory_state,
    )
    core = lax.axis_index("tp")
    half_rows = seq_count // 2
    chips = lax.axis_size("ep")
    dims = grid_of(chips)
    top_count = routing.shape[1]
    slot_cap = max(2, 2 * seq_count * top_count // chips)
    attn_sum = kept.astype(jnp.float32) + swap(sent).astype(jnp.float32)
    hidden_own = lax.dynamic_slice_in_dim(hidden, core * half_rows, half_rows, 0)
    first_res = (hidden_own.astype(jnp.float32) + attn_sum).astype(jnp.bfloat16)
    ffn_in = rms_scaled(first_res, ffn_gain).astype(jnp.bfloat16)
    notes = lax.dynamic_slice_in_dim(
        route_notes(routing, route_scale, chips), core * half_rows, half_rows, 0
    )
    rows = jnp.concatenate([ffn_in, notes], axis=1)

    near = dims[0] // 2
    line = [rows] + [hop(rows, dims, LINE, k) for k in range(1, dims[0])]
    chip = lax.axis_index("ep").astype(jnp.int32).reshape(1)
    weights = (
        expert_gate,
        expert_up,
        expert_down,
        dense_gate.T,
        dense_up.T,
        dense_down,
        blend_vector[None],
    )
    chip = touch(chip, *weights[:2])
    chip = touch(chip, *weights[2:6])
    sums = [first_res]
    for start in (0, near):
        own, other = plane_gather(jnp.stack(line[start : start + near]), dims)
        own, other = experts(own, other, slot_cap, half_rows, chip, weights)
        reduced = plane_reduce(own, other, dims)
        for k in range(near):
            if start + k:
                sums.append(hop(reduced[k], dims, LINE, -start - k))
            else:
                sums.append(reduced[k])
    out_own = total(*sums)
    out_other = swap(out_own)
    layer_out = jnp.concatenate(
        [jnp.where(core == 0, out_own, out_other), jnp.where(core == 0, out_other, out_own)]
    )
    return (layer_out, new_state)


def route_notes(routing, route_scale, chips):
    seq_count, top_count = routing.shape
    flat = routing.reshape(-1)
    one_hot = (flat[:, None] == jnp.arange(chips, dtype=jnp.int32)[None, :]).astype(jnp.int32)
    before = jnp.cumsum(one_hot, axis=0) - one_hot
    rank = jnp.sum(before * one_hot, axis=1).reshape(seq_count, top_count)
    high = route_scale.astype(jnp.bfloat16)
    low = (route_scale - high.astype(jnp.float32)).astype(jnp.bfloat16)
    fields = [routing.astype(jnp.bfloat16), rank.astype(jnp.bfloat16), high, low]
    notes = jnp.stack(fields, axis=2).reshape(seq_count, 4 * top_count)
    return jnp.pad(notes, ((0, 0), (0, 128 - 4 * top_count)))


def solution(mesh):
    in_specs = (
        P("ep", None),
        P(),
        P(None, "tp"),
        P(None, "tp"),
        P(None, "tp"),
        P(),
        P(),
        P(),
        P(),
        P(),
        P(),
        P(),
        P("tp", None),
        P("ep", "tp", None, None),
        P(),
        P(),
        P(None, ("ep", "tp")),
        P(None, ("ep", "tp")),
        P(("ep", "tp"), None),
        P("ep", None, "tp"),
        P("ep", None, "tp"),
        P("ep", "tp", None),
        P("ep", None),
        P("ep", None),
    )
    out_specs = (P("ep", None), P("ep", "tp", None, None))

    return jax.shard_map(shards, mesh=mesh, in_specs=in_specs, out_specs=out_specs, check_vma=False)
```

```python
import functools
import math

import jax
import jax.numpy as jnp
from jax import lax
from jax.experimental import pallas as pl
from jax.experimental.pallas import tpu as pltpu
from jax.sharding import PartitionSpec as P


def rms_scaled(tensor, gain_vec):
    values = tensor.astype(jnp.float32)
    return values * lax.rsqrt(jnp.mean(values * values, axis=-1, keepdims=True) + 1e-06) * gain_vec


def silu_of(tensor):
    return tensor / (1.0 + jnp.exp(-tensor))


def matmul(left, right):
    return jnp.dot(left, right, preferred_element_type=jnp.float32)


def touch_kernel(*refs):
    refs[-1][0] = refs[0][0]


def touch(chip, *values):
    smem = pl.BlockSpec(memory_space=pltpu.SMEM)
    return pl.pallas_call(
        touch_kernel,
        in_specs=[smem] + [pl.BlockSpec(memory_space=pltpu.VMEM)] * len(values),
        out_specs=smem,
        out_shape=jax.ShapeDtypeStruct(chip.shape, chip.dtype),
        compiler_params=pltpu.CompilerParams(vmem_limit_bytes=12 * 1024 * 1024),
        name="touch",
    )(chip, *values)


def experts_kernel(
    pieces,
    cap,
    span,
    chip_ref,
    expert_gate_ref,
    expert_up_ref,
    expert_down_ref,
    dense_gate_ref,
    dense_up_ref,
    dense_down_ref,
    blend_ref,
    *refs,
):
    ins, outs = refs[: len(pieces)], refs[len(pieces) : 2 * len(pieces)]
    token_scr, act_scr = refs[2 * len(pieces) :]
    width = dense_down_ref.shape[-1]
    count, _ = ins[0].shape
    slots = len(pieces) // 2 * (count // span) * cap
    named = chip_ref[0].astype(jnp.float32)
    turn = lambda left, right: lax.dot_general(
        left, right, (((1,), (1,)), ((), ())), preferred_element_type=jnp.float32
    )
    row = lax.broadcasted_iota(jnp.int32, (count, 1), 0)
    lane = lax.broadcasted_iota(jnp.int32, (count, slots), 1)
    selects, weights = [], []
    for piece, ((scale_first, scale_rest, offset, inner), ref) in enumerate(zip(pieces, ins)):
        marks = ref[:, width:].astype(jnp.float32)
        block = row // span
        base = (block // inner) * scale_first + block % inner * scale_rest + offset
        slot = jnp.full((count, 1), -1, jnp.int32)
        weight = jnp.zeros((count, 1), jnp.float32)
        for choice in range(2):
            mark = lambda k: marks[:, 4 * choice + k : 4 * choice + k + 1]
            hit = mark(0) == named
            slot = jnp.where(hit, base * cap + mark(1).astype(jnp.int32), slot)
            weight = jnp.where(hit, mark(2) + mark(3), weight)
        selects.append(jnp.where(lane == slot, 1.0, 0.0).astype(jnp.bfloat16))
        weights.append(weight)
        token_scr[piece * count : (piece + 1) * count, :] = ref[:, :width]
    select = jnp.concatenate(selects)
    picked = lax.dot_general(
        select, token_scr[...], (((0,), (0,)), ((), ())), preferred_element_type=jnp.float32
    ).astype(jnp.bfloat16)
    tokens = token_scr[...]
    blend_rows = jnp.broadcast_to(blend_ref[...], (8, width))
    blend = 1.0 / (1.0 + jnp.exp(-turn(tokens, blend_rows)[:, :1]))
    act_scr[...] = (
        silu_of(turn(tokens, dense_gate_ref[...])) * turn(tokens, dense_up_ref[...]) * blend
    ).astype(jnp.bfloat16)
    gate = silu_of(matmul(picked, expert_gate_ref[0]))
    expert_act = (gate * matmul(picked, expert_up_ref[0])).astype(jnp.bfloat16)
    expert_out = matmul(expert_act, expert_down_ref[0]).astype(jnp.bfloat16)
    for piece in range(len(pieces)):
        outs[piece][...] = (
            matmul(selects[piece], expert_out) * weights[piece]
            + matmul(act_scr[piece * count : (piece + 1) * count, :], dense_down_ref[...])
        ).astype(jnp.bfloat16)


def experts(own, other, cap, span, chip, weights):
    sides, (firsts, group, _, wide) = len(own), own[0].shape
    count = firsts * group * span
    flat = [value.reshape(count, wide) for value in own + other]
    pieces = [(group, 1, s * firsts * group, group) for s in range(sides)]
    pieces += [(firsts * group, 1, s * group, group) for s in range(sides)]
    width = weights[2].shape[-1]
    vmem = pl.BlockSpec(memory_space=pltpu.VMEM)
    units = weights[0].shape[-1]
    rows = 2 * sides * count
    outs = pl.pallas_call(
        functools.partial(experts_kernel, tuple(pieces), cap, span),
        in_specs=[pl.BlockSpec(memory_space=pltpu.SMEM)] + [vmem] * (len(weights) + len(flat)),
        out_specs=[vmem] * len(flat),
        out_shape=[jax.ShapeDtypeStruct((count, width), jnp.bfloat16)] * len(flat),
        scratch_shapes=[
            pltpu.VMEM((rows, width), jnp.bfloat16),
            pltpu.VMEM((rows, weights[3].shape[0]), jnp.bfloat16),
        ],
        compiler_params=pltpu.CompilerParams(vmem_limit_bytes=16 * 1024 * 1024 + rows * 24000),
        cost_estimate=pl.CostEstimate(
            flops=6 * rows * width * 2 * units, bytes_accessed=6 * width * units, transcendentals=0
        ),
        name="experts",
    )(chip, *weights, *flat)
    outs = [value.reshape(firsts, group, span, width) for value in outs]
    return outs[:sides], outs[sides:]


def grid_of(count):
    side = max(1, int(round((count / 4) ** 0.5)))
    if 4 * side * side == count:
        return (4, side, side)
    return (count, 1, 1)


def turned(index, dims, axis, step):
    place = [index // (dims[1] * dims[2]), index // dims[2] % dims[1], index % dims[2]]
    place[axis] = (place[axis] + step) % dims[axis]
    return (place[0] * dims[1] + place[1]) * dims[2] + place[2]


def hop(value, dims, axes, step):
    count = dims[0] * dims[1] * dims[2]
    perm = [
        (2 * chip + core, 2 * turned(chip, dims, axes[core], step) + core)
        for chip in range(count)
        for core in range(2)
    ]
    return lax.ppermute(value, ("ep", "tp"), perm)


def swap(value):
    return lax.ppermute(value, "tp", [(0, 1), (1, 0)])


LINE, FIRST, SECOND = (0, 0), (2, 1), (1, 2)


def total(*values):
    return sum(value.astype(jnp.float32) for value in values).astype(jnp.bfloat16)


def plane_gather(blocks, dims):
    near = range(1, dims[1])
    firsts = jnp.stack([blocks] + [hop(blocks, dims, FIRST, k) for k in near])
    own = [firsts] + [hop(firsts, dims, SECOND, k) for k in near]
    other = [swap(own[0])]
    return own, other + [swap(value) for value in own[1:]]


def plane_reduce(own, other, dims):
    near = range(1, dims[1])
    back = [swap(other[k]) for k in near]
    back = [swap(other[0])] + back
    arrived = [hop(total(own[k], back[k]), dims, SECOND, -k) for k in near]
    firsts = total(own[0], back[0], *arrived)
    return total(firsts[0], *[hop(firsts[k], dims, FIRST, -k) for k in near])


def attention_kernel(
    core_ref,
    hidden_ref,
    mix_ref,
    recept_ref,
    key_ref,
    value_ref,
    decay_down_ref,
    decay_up_ref,
    decay_bias_ref,
    rate_down_ref,
    rate_up_ref,
    rate_bias_ref,
    gain_ref,
    out_weight_ref,
    state_ref,
    kept_ref,
    sent_ref,
    new_ref,
    unit_scr,
    pull_scr,
    push_scr,
    decay_scr,
    recept_scr,
    value_scr,
    head_scr,
):
    heads, seqs, size = unit_scr.shape
    block = state_ref.shape[0]
    step = pl.program_id(0)

    def flat_dot(left, right):
        return lax.dot_general(
            left, right, (((1,), (1,)), ((), ())), preferred_element_type=jnp.float32
        )

    @pl.when(step == 0)
    def _():
        normed = rms_scaled(hidden_ref[...], mix_ref[...]).astype(jnp.bfloat16)
        rounded = lambda value: value.astype(jnp.bfloat16).astype(jnp.float32)
        recept = rounded(matmul(normed, recept_ref[...]))
        key = rounded(matmul(normed, key_ref[...]))
        value = rounded(matmul(normed, value_ref[...]))
        decay_low = jnp.tanh(flat_dot(normed, decay_down_ref[...])).astype(jnp.bfloat16)
        decay_pre = matmul(decay_low, decay_up_ref[...]) + decay_bias_ref[...]
        decay = jnp.exp(-math.exp(-0.5) / (1.0 + jnp.exp(-decay_pre)))
        rate_low = flat_dot(normed, rate_down_ref[...]).astype(jnp.bfloat16)
        rate = 1.0 / (1.0 + jnp.exp(-(matmul(rate_low, rate_up_ref[...]) + rate_bias_ref[...])))
        for head in range(heads):
            cut = slice(head * size, (head + 1) * size)
            own_key = key[:, cut]
            unit = own_key * lax.rsqrt(
                jnp.sum(own_key * own_key, axis=-1, keepdims=True) + 1e-06
            )
            unit_scr[head] = unit
            pull_scr[head] = unit * rate[:, cut]
            push_scr[head] = own_key * rate[:, cut]
            decay_scr[head] = decay[:, cut]
            recept_scr[head] = recept[:, cut]
            value_scr[head] = value[:, cut]

    rows = pl.ds(pl.multiple_of(step * block, block), block)
    ones = jnp.ones((size, 128), jnp.bfloat16)
    lane = lax.broadcasted_iota(jnp.int32, (size, 128), 1)

    own = lax.broadcasted_iota(jnp.int32, (size, 2 * block), 1) % block
    blank = jnp.zeros((block, size), jnp.float32)

    def pulled(head):
        unit = jnp.concatenate([unit_scr[head, rows, :], blank]).astype(jnp.bfloat16)
        states = [state_ref[seq, head].astype(jnp.bfloat16) for seq in range(block)]
        return flat_dot(jnp.concatenate(states), unit)

    def updated(head, removed):
        decay = decay_scr[head, rows, :]
        recept = recept_scr[head, rows, :]
        upright = jnp.concatenate([blank, value_scr[head, rows, :]]).T
        factors = [
            jnp.where(own == seq, removed[seq * size : (seq + 1) * size] + upright, 0.0)
            for seq in range(block)
        ]
        changes = jnp.concatenate([-pull_scr[head, rows, :], push_scr[head, rows, :]])
        change = matmul(
            jnp.concatenate(factors).astype(jnp.bfloat16), changes.astype(jnp.bfloat16)
        )
        products = []
        for seq in range(block):
            one = slice(seq, seq + 1)
            fresh = state_ref[seq, head] * decay[one] + change[seq * size : (seq + 1) * size]
            new_ref[seq, head] = fresh
            products.append((fresh * recept[one]).astype(jnp.bfloat16))
        return matmul(jnp.concatenate(products), ones)

    def normed(head, readout):
        columns = jnp.zeros((size, 128), jnp.float32)
        for seq in range(block):
            columns = jnp.where(lane == seq, readout[seq * size : (seq + 1) * size], columns)
        lines = columns.T[:block]
        centred = lines - jnp.mean(lines, axis=-1, keepdims=True)
        variance = jnp.mean(centred * centred, axis=-1, keepdims=True)
        head_scr[head, rows, :] = (
            centred
            * lax.rsqrt(variance + 0.00064)
            * gain_ref[:, head * size : (head + 1) * size]
        )

    removed = pulled(0)
    readout = None
    for head in range(heads):
        following = pulled(head + 1) if head + 1 < heads else None
        finished = updated(head, removed)
        if head:
            normed(head - 1, readout)
        removed, readout = following, finished
    normed(heads - 1, readout)

    @pl.when(step == pl.num_programs(0) - 1)
    def _():
        half = seqs // 2
        for side, ref in ((core_ref[0], kept_ref), (1 - core_ref[0], sent_ref)):
            picked = pl.ds(pl.multiple_of(side * half, half), half)
            lines = jnp.concatenate([head_scr[head, picked, :] for head in range(heads)], axis=1)
            ref[...] = matmul(lines.astype(jnp.bfloat16), out_weight_ref[...]).astype(ref.dtype)


def attention(
    hidden,
    mix_gain,
    recept_weight,
    key_weight,
    value_weight,
    decay_down,
    decay_up,
    decay_bias,
    rate_down,
    rate_up,
    rate_bias,
    head_gain,
    out_weight,
    memory_state,
):
    seqs, width = hidden.shape
    _, heads, size, _ = memory_state.shape
    own = heads * size
    low = decay_down.shape[1]
    block = 8
    core = lax.axis_index("tp").astype(jnp.int32).reshape(1)
    whole = lambda *shape: pl.BlockSpec(shape, lambda i, c: (0,) * len(shape))
    half = lambda rows: pl.BlockSpec((rows, own), lambda i, c: (0, c[0]))
    state_spec = pl.BlockSpec((block, heads, size, size), lambda i, c: (i, 0, 0, 0))
    per_head = pltpu.VMEM((heads, seqs, size), jnp.float32)
    return pl.pallas_call(
        attention_kernel,
        grid_spec=pltpu.PrefetchScalarGridSpec(
            num_scalar_prefetch=1,
            grid=(seqs // block,),
            in_specs=[
                whole(seqs, width),
                whole(1, width),
                whole(width, own),
                whole(width, own),
                whole(width, own),
                whole(low, width),
                half(low),
                half(1),
                whole(low, width),
                half(low),
                half(1),
                half(1),
                whole(own, width),
                state_spec,
            ],
            out_specs=[whole(seqs // 2, width), whole(seqs // 2, width), state_spec],
            scratch_shapes=[per_head] * 7,
        ),
        out_shape=[
            jax.ShapeDtypeStruct((seqs // 2, width), jnp.bfloat16),
            jax.ShapeDtypeStruct((seqs // 2, width), jnp.bfloat16),
            jax.ShapeDtypeStruct(memory_state.shape, memory_state.dtype),
        ],
        compiler_params=pltpu.CompilerParams(
            dimension_semantics=("arbitrary",), vmem_limit_bytes=66000000
        ),
        name="attention",
    )(
        core,
        hidden,
        mix_gain[None],
        recept_weight,
        key_weight,
        value_weight,
        decay_down.T,
        decay_up,
        decay_bias[None],
        rate_down.T,
        rate_up,
        rate_bias[None],
        head_gain[None],
        out_weight,
        memory_state,
    )


def shards(
    hidden,
    mix_gain,
    recept_weight,
    key_weight,
    value_weight,
    decay_down,
    decay_up,
    decay_bias,
    rate_down,
    rate_up,
    rate_bias,
    head_gain,
    out_weight,
    memory_state,
    ffn_gain,
    blend_vector,
    dense_gate,
    dense_up,
    dense_down,
    expert_gate,
    expert_up,
    expert_down,
    routing,
    route_scale,
):
    seq_count, _ = hidden.shape
    kept, sent, new_state = attention(
        hidden,
        mix_gain,
        recept_weight,
        key_weight,
        value_weight,
        decay_down,
        decay_up,
        decay_bias,
        rate_down,
        rate_up,
        rate_bias,
        head_gain,
        out_weight,
        memory_state,
    )
    core = lax.axis_index("tp")
    half_rows = seq_count // 2
    chips = lax.axis_size("ep")
    dims = grid_of(chips)
    top_count = routing.shape[1]
    slot_cap = max(2, 2 * seq_count * top_count // chips)
    attn_sum = kept.astype(jnp.float32) + swap(sent).astype(jnp.float32)
    hidden_own = lax.dynamic_slice_in_dim(hidden, core * half_rows, half_rows, 0)
    first_res = (hidden_own.astype(jnp.float32) + attn_sum).astype(jnp.bfloat16)
    ffn_in = rms_scaled(first_res, ffn_gain).astype(jnp.bfloat16)
    notes = lax.dynamic_slice_in_dim(
        route_notes(routing, route_scale, chips), core * half_rows, half_rows, 0
    )
    rows = jnp.concatenate([ffn_in, notes], axis=1)

    near = dims[0] // 2
    line = [rows] + [hop(rows, dims, LINE, k) for k in range(1, dims[0])]
    chip = lax.axis_index("ep").astype(jnp.int32).reshape(1)
    weights = (
        expert_gate,
        expert_up,
        expert_down,
        dense_gate.T,
        dense_up.T,
        dense_down,
        blend_vector[None],
    )
    chip = touch(chip, *weights[:2])
    chip = touch(chip, *weights[2:6])
    sums = [first_res]
    for start in (0, near):
        own, other = plane_gather(jnp.stack(line[start : start + near]), dims)
        own, other = experts(own, other, slot_cap, half_rows, chip, weights)
        reduced = plane_reduce(own, other, dims)
        for k in range(near):
            if start + k:
                sums.append(hop(reduced[k], dims, LINE, -start - k))
            else:
                sums.append(reduced[k])
    out_own = total(*sums)
    out_other = swap(out_own)
    layer_out = jnp.concatenate(
        [jnp.where(core == 0, out_own, out_other), jnp.where(core == 0, out_other, out_own)]
    )
    return (layer_out, new_state)


def route_notes(routing, route_scale, chips):
    seq_count, top_count = routing.shape
    flat = routing.reshape(-1)
    one_hot = (flat[:, None] == jnp.arange(chips, dtype=jnp.int32)[None, :]).astype(jnp.int32)
    before = jnp.cumsum(one_hot, axis=0) - one_hot
    rank = jnp.sum(before * one_hot, axis=1).reshape(seq_count, top_count)
    high = route_scale.astype(jnp.bfloat16)
    low = (route_scale - high.astype(jnp.float32)).astype(jnp.bfloat16)
    fields = [routing.astype(jnp.bfloat16), rank.astype(jnp.bfloat16), high, low]
    notes = jnp.stack(fields, axis=2).reshape(seq_count, 4 * top_count)
    return jnp.pad(notes, ((0, 0), (0, 128 - 4 * top_count)))


def solution(mesh):
    in_specs = (
        P("ep", None),
        P(),
        P(None, "tp"),
        P(None, "tp"),
        P(None, "tp"),
        P(),
        P(),
        P(),
        P(),
        P(),
        P(),
        P(),
        P("tp", None),
        P("ep", "tp", None, None),
        P(),
        P(),
        P(None, ("ep", "tp")),
        P(None, ("ep", "tp")),
        P(("ep", "tp"), None),
        P("ep", None, "tp"),
        P("ep", None, "tp"),
        P("ep", "tp", None),
        P("ep", None),
        P("ep", None),
    )
    out_specs = (P("ep", None), P("ep", "tp", None, None))

    return jax.shard_map(shards, mesh=mesh, in_specs=in_specs, out_specs=out_specs, check_vma=False)
```
